256 devices in a mesh: fs: 16 (over y, x), tp: 16 (over z, core).
Axes of the slice: x: 4, y: 4, z: 8, core: 2. Of those that a mesh axis runs over, the one named last changes fastest.
Arguments:
- stream_in: bfloat16 [32768, 4096], P(('fs', 'tp')), may hold values from -6 to 6
- mixer_out: bfloat16 [32768, 4096], P(('fs', 'tp')), may hold values from -6 to 6
- mix_gain: float32 [4096], replicated, may hold values from 0.1 to 1.9
- pre_gain: float32 [4096], replicated, may hold values from 0.1 to 1.9
- gate_weight: float32 [4096, 6144], P('fs', 'tp'), may hold values from -0.09375 to 0.09375
- up_weight: float32 [4096, 6144], P('fs', 'tp'), may hold values from -0.09375 to 0.09375
- gate_scale: float32 [6144], P('tp'), may hold values from 0.5 to 2
- up_scale: float32 [6144], P('tp'), may hold values from 0.5 to 2
Outputs:
- hidden: bfloat16 [32768, 6144], P('fs', 'tp')
- stream: bfloat16 [32768, 4096], P(('fs', 'tp'))
The draws below stay inside these ranges and needn't reach their ends.
All inputs are finite; a program needn't handle non-finite values.
Results may differ from the reference program's by a relative error of at most 0.0082.
Values may be sent and summed in bfloat16 or wider, within the bound.
A program may use at most 128 MiB of HBM per device.

```python
import math
import jax
import jax.numpy as jnp
from jax import lax

D = 4096
FF = 6144
TOKENS = 32768


def levels(rng, shape, split, low, largest):
    def one(dim, shards_of):
        steps = jax.random.uniform(jax.random.fold_in(jax.random.fold_in(rng, 6), dim), (shards_of,), jnp.float32, low / len(split), largest / len(split))
        return jnp.repeat(jnp.exp(steps), shape[dim] // shards_of).reshape((-1,) + (1,) * (len(shape) - dim - 1))

    level = one(*split[0])
    for cut in split[1:]:
        level = level * one(*cut)
    return level


def centred(key, extent, width, limit, pieces=(), kind=jnp.bfloat16):
    entries = jax.random.normal(key, extent, jnp.float32) * width
    if len(pieces) > 0:
        entries = levels(key, extent, pieces, -0.22, 0.18) * entries
    return jnp.clip(entries, min=-limit, max=limit).astype(kind)


def setup_inputs(seed: int = 0) -> dict:
    splits = jax.random.split(jax.random.key(seed), 9)
    stream_in = centred(splits[0], (TOKENS, D), 1.0, 6.0, ((0, 256),))
    mixer_out = centred(splits[1], (TOKENS, D), 1.0, 6.0, ((0, 256),))
    mix_gain = jnp.clip(1.0 + 0.18 * jax.random.normal(splits[2], (D,), jnp.float32), 0.1, 1.9)
    pre_gain = jnp.clip(1.0 + 0.18 * jax.random.normal(splits[3], (D,), jnp.float32), 0.1, 1.9)
    gate_weight = centred(splits[4], (D, FF), D ** -0.5, 0.09375, ((0, 16), (1, 16)), jnp.float32)
    up_weight = centred(splits[5], (D, FF), D ** -0.5, 0.09375, ((0, 16), (1, 16)), jnp.float32)
    gate_scale = jnp.clip(jnp.exp(math.log(2.0) - 1.3862944 * jax.random.uniform(splits[6], (FF,), jnp.float32) ** levels(splits[6], (FF,), ((0, 16),), -0.2, 0.2)), 0.5, 2.0)
    up_scale = jnp.clip(jnp.exp(math.log(2.0) - 1.3862944 * jax.random.uniform(splits[7], (FF,), jnp.float32) ** levels(splits[7], (FF,), ((0, 16),), -0.2, 0.2)), 0.5, 2.0)
    return {"stream_in": stream_in, "mixer_out": mixer_out, "mix_gain": mix_gain, "pre_gain": pre_gain, "gate_weight": gate_weight, "up_weight": up_weight, "gate_scale": gate_scale, "up_scale": up_scale}


epsilon = 1e-06

def rms_scaled(values, gain):
    return values * lax.rsqrt(lax.optimization_barrier(jnp.mean(values * values, axis=-1, keepdims=True)) + epsilon) * gain

def reference(stream_in, mixer_out, mix_gain, pre_gain, gate_weight, up_weight, gate_scale, up_scale):
    mixed = stream_in.astype(jnp.float32) + rms_scaled(mixer_out.astype(jnp.float32), mix_gain)
    stream = mixed.astype(jnp.bfloat16)
    normed = rms_scaled(stream.astype(jnp.float32), pre_gain).astype(jnp.bfloat16)
    gate = jnp.dot(normed, gate_weight.astype(jnp.bfloat16), preferred_element_type=jnp.float32) * gate_scale
    up = jnp.dot(normed, up_weight.astype(jnp.bfloat16), preferred_element_type=jnp.float32) * up_scale
    hidden = (jax.nn.silu(gate) * up).astype(jnp.bfloat16)
    return (hidden, stream)
```

```python
import functools

import jax
import jax.numpy as jnp
from jax import lax
from jax.experimental import pallas as pl
from jax.experimental.pallas import tpu as pltpu
from jax.sharding import PartitionSpec as P

MESH = pl.DeviceIdType.MESH
epsilon = 1e-06

D = 4096
ROWS = 128
COLS = 384
SIDE = 4
DEEP = 8
SHARD = 256
HALF = SHARD // 2
QUARTER = HALF // 2
CHUNK = 32
CHUNKS = ROWS // CHUNK
LANES = 512
TILES = COLS // 128
F32 = jnp.float32
BF16 = jnp.bfloat16


def kernel(
    stream_in, mixer_out, mix_gain, pre_gain, gate_w, up_w, gate_s, up_s,
    hidden, stream,
    tok, w, stream_v, mixer_v, stream_o, gate_v, up_v, mg, pg, gs, us, hid,
    in_sem, out_sem, zs, zr, ds_, dr, ws, wr,
):
    fs, tp = lax.axis_index("fs"), lax.axis_index("tp")
    x, y = lax.rem(fs, SIDE), lax.div(fs, SIDE)
    core, z = lax.rem(tp, 2), lax.div(tp, 2)

    def up_by(v, k, n):
        return lax.rem(v + k, n)

    along_z = {s: (fs, up_by(z, k, DEEP) * 2 + core) for s, k in ((0, 1), (1, DEEP - 1))}
    partner = (fs, z * 2 + (1 - core))
    along = {
        ("x", 0): (y * SIDE + up_by(x, 1, SIDE), tp),
        ("x", 1): (y * SIDE + up_by(x, SIDE - 1, SIDE), tp),
        ("y", 0): (up_by(y, 1, SIDE) * SIDE + x, tp),
        ("y", 1): (up_by(y, SIDE - 1, SIDE) * SIDE + x, tp),
    }
    neighbours = list(along_z.values()) + [partner] + list(along.values())

    loads = {}

    def load(name, src, dst):
        c = pltpu.make_async_copy(src, dst, in_sem.at[len(loads)])
        c.start()
        loads[name] = c

    load("mg", mix_gain, mg)
    load("pg", pre_gain, pg)
    for c in range(CHUNKS):
        rows = pl.ds(c * CHUNK, CHUNK)
        load(("m", c), mixer_out.at[rows], mixer_v.at[rows])
        load(("s", c), stream_in.at[rows], stream_v.at[rows])
        if c == 0:
            load("gw", gate_w, gate_v)
            load("uw", up_w, up_v)
    load("gs", gate_s, gs)
    load("us", up_s, us)

    barrier = pltpu.get_barrier_semaphore()
    for n in neighbours:
        pl.semaphore_signal(barrier, inc=1, device_id=n, device_id_type=MESH)

    def norm(c):
        loads[("m", c)].wait()
        loads[("s", c)].wait()

        def some(i, carry):
            rows = pl.ds(pl.multiple_of(c * CHUNK + i * 16, 16), 16)
            parts = [pl.ds(k * LANES, LANES) for k in range(D // LANES)]
            total = jnp.zeros((16, LANES), F32)
            for p in parts:
                m = mixer_v[rows, p].astype(F32)
                total += m * m
            inv = lax.rsqrt(jnp.sum(total, axis=-1, keepdims=True) * (1.0 / D) + epsilon)
            total = jnp.zeros((16, LANES), F32)
            for p in parts:
                m = mixer_v[rows, p].astype(F32)
                s = (stream_v[rows, p].astype(F32) + m * inv * mg[:, p]).astype(BF16)
                stream_o[rows, p] = s
                s = s.astype(F32)
                total += s * s
            inv = lax.rsqrt(jnp.sum(total, axis=-1, keepdims=True) * (1.0 / D) + epsilon)
            for p in parts:
                s = stream_o[rows, p].astype(F32)
                tok[0, rows, p] = (s * inv * pg[:, p]).astype(BF16)
            return carry

        lax.fori_loop(0, CHUNK // 16, some, 0)

    sent = []

    def send(src, dst, ssem, rsem, device):
        c = pltpu.make_async_remote_copy(
            src_ref=src, dst_ref=dst, send_sem=ssem, recv_sem=rsem,
            device_id=device, device_id_type=MESH,
        )
        c.start()
        sent.append(c)

    def arrived(dst, ssem, rsem):
        pltpu.make_async_remote_copy(
            src_ref=dst, dst_ref=dst, send_sem=ssem, recv_sem=rsem,
            device_id=partner, device_id_type=MESH,
        ).wait_recv()

    def piece(dz, which, c):
        return tok.at[dz, pl.ds(which * ROWS + c * CHUNK, CHUNK)]

    def z_index(dz, c):
        return (dz - 1) * CHUNKS + c

    def z_send(way, dz, c):
        if dz >= DEEP // 2 or (dz == DEEP // 2 - 1 and (c < CHUNKS // 2) == (way == 1)):
            return
        here, there = (dz, dz + 1) if way == 0 else (-dz % DEEP, DEEP - 1 - dz)
        i = z_index(dz + 1, c)
        send(piece(here, 0, c), piece(there, 0, c), zs.at[way, i], zr.at[way, i], along_z[way])

    def d_send(dz, c):
        i = dz * CHUNKS + c
        send(piece(dz, 0, c), piece(dz, 1, c), ds_.at[i], dr.at[i], partner)

    def z_take(way, steps, c):
        i = z_index(steps, c)
        dz = steps if way == 0 else DEEP - steps
        arrived(piece(dz, 0, c), zs.at[way, i], zr.at[way, i])
        z_send(way, steps, c)
        d_send(dz, c)

    def d_take(dz, c):
        i = dz * CHUNKS + c
        arrived(piece(dz, 1, c), ds_.at[i], dr.at[i])

    rings = {"A": ("x", 0, 0, 0), "B": ("y", 0, 1, 1)}
    for j in range(SIDE):
        rings[("A", j)] = ("y", j, 0, 2 + j)
        rings[("B", j)] = ("x", j, 1, 2 + SIDE + j)

    def w_rows(ring, step, start, count):
        axis, j, half, _ = rings[ring]
        dx, dy = (step, j) if axis == "x" else (j, step)
        owner = up_by(y, SIDE - dy, SIDE) * SIDE + up_by(x, SIDE - dx, SIDE)
        return w.at[pl.ds(pl.multiple_of(owner * SHARD + half * HALF + start, QUARTER), count)]

    def w_send(ring, step, start, count, way, i):
        axis, _, _, r = rings[ring]
        ref = w_rows(ring, step, start, count)
        send(ref, ref, ws.at[r, i], wr.at[r, i], along[(axis, way)])

    def w_begin(ring):
        w_send(ring, 0, 0, HALF, 0, 0)
        w_send(ring, 0, 0, HALF, 1, 1)

    def w_near(ring):
        r = rings[ring][3]
        arrived(w_rows(ring, 1, 0, HALF), ws.at[r, 0], wr.at[r, 0])
        w_send(ring, 1, 0, QUARTER, 0, 2)
        arrived(w_rows(ring, SIDE - 1, 0, HALF), ws.at[r, 1], wr.at[r, 1])
        w_send(ring, SIDE - 1, QUARTER, QUARTER, 1, 3)

    def w_far(ring):
        r = rings[ring][3]
        arrived(w_rows(ring, 2, 0, QUARTER), ws.at[r, 2], wr.at[r, 2])
        arrived(w_rows(ring, 2, QUARTER, QUARTER), ws.at[r, 3], wr.at[r, 3])

    outs = []

    def row_of(dz, which):
        owner = up_by(z, DEEP - dz, DEEP) * 2 + (core if which == 0 else 1 - core)
        return owner * ROWS

    def project(dz, spans):
        def tile(j, carry):
            cols = pl.ds(pl.multiple_of(j * 256, 256), 256)
            mine = pl.ds(pl.multiple_of(j * 128, 128), 128)
            parts = [tok[dz, pl.ds(a, n), :] for a, n in spans]
            lhs = parts[0] if len(parts) == 1 else jnp.concatenate(parts, axis=0)
            both = jnp.dot(lhs, w[:, cols], preferred_element_type=F32)
            gate = both[:, :128] * gs[:, mine]
            up = both[:, 128:] * us[:, mine]
            out = (gate / (1.0 + jnp.exp(-gate)) * up).astype(BF16)
            at = 0
            for a, n in spans:
                hid[dz, pl.ds(a, n), mine] = out[at:at + n]
                at += n
            return carry

        lax.fori_loop(0, TILES, tile, 0)
        for a, n in spans:
            first = a
            while first < a + n:
                which = first // ROWS
                size = min(a + n, (which + 1) * ROWS) - first
                to = pl.multiple_of(row_of(dz, which) + first % ROWS, CHUNK)
                c = pltpu.make_async_copy(
                    hid.at[dz, pl.ds(first, size)],
                    hidden.at[pl.ds(to, size)],
                    out_sem.at[len(outs)],
                )
                c.start()
                outs.append(c)
                first += size

    loads["mg"].wait()
    loads["pg"].wait()
    loads["gw"].wait()
    loads["uw"].wait()
    own = pl.ds(pl.multiple_of(fs * SHARD, SHARD), SHARD)
    for j in range(TILES):
        w[own, j * 256:j * 256 + 128] = gate_v[:, j * 128:(j + 1) * 128].astype(BF16)
        w[own, j * 256 + 128:(j + 1) * 256] = up_v[:, j * 128:(j + 1) * 128].astype(BF16)

    def own_out(c):
        z_send(0, 0, c)
        z_send(1, 0, c)
        d_send(0, c)

    norm(0)
    pl.semaphore_wait(barrier, len(neighbours))
    w_begin("A")
    w_begin("B")
    w_begin(("A", 0))
    w_begin(("B", 0))
    for c in range(1, CHUNKS):
        norm(c)
        own_out(c - 1)
    loads["gs"].wait()
    loads["us"].wait()
    c = pltpu.make_async_copy(stream_o, stream, out_sem.at[0])
    c.start()
    outs.append(c)
    own_out(CHUNKS - 1)

    def z_both(steps, c):
        z_take(0, steps, c)
        z_take(1, steps, c)

    w_near("A")
    w_near("B")
    for r in ("A", "B"):
        w_begin((r, 1))
        w_begin((r, 3))
    z_both(1, 0)
    w_near(("A", 0))
    w_near(("B", 0))
    w_far("A")
    w_far("B")
    w_begin(("A", 2))
    w_begin(("B", 2))
    z_both(1, 1)
    w_near(("A", 1))
    w_near(("B", 1))
    z_both(1, 2)
    w_near(("A", 3))
    w_near(("B", 3))
    w_far(("A", 0))
    w_far(("B", 0))
    z_both(1, 3)
    w_near(("A", 2))
    w_near(("B", 2))
    for j in (1, 3):
        w_far(("A", j))
        w_far(("B", j))
    z_both(2, 0)
    w_far(("A", 2))
    w_far(("B", 2))

    def whole(dz):
        for c in range(CHUNKS):
            d_take(dz, c)
        project(dz, ((0, 2 * ROWS),))

    whole(0)
    whole(1)
    z_both(2, 1)
    whole(DEEP - 1)
    z_both(2, 2)
    z_both(2, 3)
    whole(2)
    z_both(3, 0)
    whole(DEEP - 2)
    z_both(3, 1)
    z_both(3, 2)
    z_both(3, 3)
    whole(3)
    whole(DEEP - 3)
    far = DEEP // 2
    for c in range(CHUNKS // 2):
        cs = (c, c + CHUNKS // 2)
        z_take(0, far, cs[0])
        z_take(1, far, cs[1])
        for k in cs:
            d_take(far, k)
        project(far, tuple((h * ROWS + k * CHUNK, CHUNK) for h in (0, 1) for k in cs))

    for c in sent:
        c.wait_send()
    for c in outs:
        c.wait()


def on_device(
    stream_in, mixer_out, mix_gain, pre_gain, gate_weight, up_weight, gate_scale, up_scale
):
    any_ = pl.BlockSpec(memory_space=pltpu.HBM)
    dma = pltpu.SemaphoreType.DMA
    z_copies = (DEEP // 2) * CHUNKS
    return pl.pallas_call(
        kernel,
        name="gathered_projections",
        out_shape=(
            jax.ShapeDtypeStruct((DEEP * 2 * ROWS, COLS), BF16),
            jax.ShapeDtypeStruct((ROWS, D), BF16),
        ),
        in_specs=[any_] * 8,
        out_specs=(any_, any_),
        scratch_shapes=[
            pltpu.VMEM((DEEP, 2 * ROWS, D), BF16),
            pltpu.VMEM((D, 2 * COLS), BF16),
            pltpu.VMEM((ROWS, D), BF16),
            pltpu.VMEM((ROWS, D), BF16),
            pltpu.VMEM((ROWS, D), BF16),
            pltpu.VMEM((SHARD, COLS), F32),
            pltpu.VMEM((SHARD, COLS), F32),
            pltpu.VMEM((1, D), F32),
            pltpu.VMEM((1, D), F32),
            pltpu.VMEM((1, COLS), F32),
            pltpu.VMEM((1, COLS), F32),
            pltpu.VMEM((DEEP, 2 * ROWS, COLS), BF16),
            dma((6 + 2 * CHUNKS,)),
            dma((64,)),
            dma((2, z_copies)),
            dma((2, z_copies)),
            dma((DEEP * CHUNKS,)),
            dma((DEEP * CHUNKS,)),
            dma((2 + 2 * SIDE, 4)),
            dma((2 + 2 * SIDE, 4)),
        ],
        compiler_params=pltpu.CompilerParams(
            collective_id=0, has_side_effects=True, vmem_limit_bytes=56 * 2**20
        ),
    )(
        stream_in, mixer_out, mix_gain.reshape(1, -1), pre_gain.reshape(1, -1),
        gate_weight, up_weight, gate_scale.reshape(1, -1), up_scale.reshape(1, -1),
    )


def solution(mesh):
    return jax.shard_map(
        on_device,
        mesh=mesh,
        in_specs=(
            P(("fs", "tp"), None),
            P(("fs", "tp"), None),
            P(),
            P(),
            P("fs", "tp"),
            P("fs", "tp"),
            P("tp"),
            P("tp"),
        ),
        out_specs=(P("fs", "tp"), P(("fs", "tp"), None)),
        check_vma=False,
    )
```

```python
import functools

import jax
import jax.numpy as jnp
from jax import lax
from jax.experimental import pallas as pl
from jax.experimental.pallas import tpu as pltpu
from jax.sharding import PartitionSpec as P

MESH = pl.DeviceIdType.MESH
epsilon = 1e-06

D = 4096
ROWS = 128
COLS = 384
SIDE = 4
DEEP = 8
SHARD = 256
HALF = SHARD // 2
QUARTER = HALF // 2
CHUNK = 32
CHUNKS = ROWS // CHUNK
FAR = ((0, 32), (32, 16), (48, 16))
LANES = 512
TILES = COLS // 128
F32 = jnp.float32
BF16 = jnp.bfloat16


def kernel(
    stream_in, mixer_out, mix_gain, pre_gain, gate_w, up_w, gate_s, up_s,
    hidden, stream,
    tok, w, stream_v, mixer_v, gate_v, up_v, mg, pg, gs, us, scales,
    in_sem, zs, zr, ds_, dr, ws, wr,
):
    fs, tp = lax.axis_index("fs"), lax.axis_index("tp")
    x, y = lax.rem(fs, SIDE), lax.div(fs, SIDE)
    core, z = lax.rem(tp, 2), lax.div(tp, 2)

    def up_by(v, k, n):
        return lax.rem(v + k, n)

    along_z = {s: (fs, up_by(z, k, DEEP) * 2 + core) for s, k in ((0, 1), (1, DEEP - 1))}
    partner = (fs, z * 2 + (1 - core))
    along = {
        ("x", 0): (y * SIDE + up_by(x, 1, SIDE), tp),
        ("x", 1): (y * SIDE + up_by(x, SIDE - 1, SIDE), tp),
        ("y", 0): (up_by(y, 1, SIDE) * SIDE + x, tp),
        ("y", 1): (up_by(y, SIDE - 1, SIDE) * SIDE + x, tp),
    }
    neighbours = list(along_z.values()) + [partner] + list(along.values())

    loads = {}

    def load(name, src, dst):
        c = pltpu.make_async_copy(src, dst, in_sem.at[len(loads)])
        c.start()
        loads[name] = c

    load("mg", mix_gain, mg)
    load("pg", pre_gain, pg)
    for c in range(CHUNKS):
        rows = pl.ds(c * CHUNK, CHUNK)
        load(("m", c), mixer_out.at[rows], mixer_v.at[rows])
        load(("s", c), stream_in.at[rows], stream_v.at[rows])
        if c == 0:
            load("gw", gate_w, gate_v)
            load("uw", up_w, up_v)
    load("gs", gate_s, gs)
    load("us", up_s, us)

    barrier = pltpu.get_barrier_semaphore()
    for n in neighbours:
        pl.semaphore_signal(barrier, inc=1, device_id=n, device_id_type=MESH)

    def norm(c):
        loads[("m", c)].wait()
        loads[("s", c)].wait()

        def some(i, carry):
            rows = pl.ds(pl.multiple_of(c * CHUNK + i * 16, 16), 16)
            parts = [pl.ds(k * LANES, LANES) for k in range(D // LANES)]
            total = jnp.zeros((16, LANES), F32)
            for p in parts:
                m = mixer_v[rows, p].astype(F32)
                total += m * m
            inv = lax.rsqrt(jnp.sum(total, axis=-1, keepdims=True) * (1.0 / D) + epsilon)
            total = jnp.zeros((16, LANES), F32)
            for p in parts:
                m = mixer_v[rows, p].astype(F32)
                s = (stream_v[rows, p].astype(F32) + m * inv * mg[:, p]).astype(BF16)
                stream[rows, p] = s
                s = s.astype(F32)
                total += s * s
            inv = lax.rsqrt(jnp.sum(total, axis=-1, keepdims=True) * (1.0 / D) + epsilon)
            for p in parts:
                s = stream[rows, p].astype(F32)
                tok[0, rows, p] = (s * inv * pg[:, p]).astype(BF16)
            return carry

        lax.fori_loop(0, CHUNK // 16, some, 0)

    sent = []

    def send(src, dst, ssem, rsem, device):
        c = pltpu.make_async_remote_copy(
            src_ref=src, dst_ref=dst, send_sem=ssem, recv_sem=rsem,
            device_id=device, device_id_type=MESH,
        )
        c.start()
        sent.append(c)

    def arrived(dst, ssem, rsem):
        pltpu.make_async_remote_copy(
            src_ref=dst, dst_ref=dst, send_sem=ssem, recv_sem=rsem,
            device_id=partner, device_id_type=MESH,
        ).wait_recv()

    far = DEEP // 2

    def piece(dz, which, rows):
        return tok.at[dz, pl.ds(which * ROWS + rows[0], rows[1])]

    def chunk(c):
        return (c * CHUNK, CHUNK)

    def far_piece(way, k):
        return (way * (ROWS // 2) + FAR[k][0], FAR[k][1])

    def z_send(way, steps, rows, i):
        here, there = (steps, steps + 1) if way == 0 else (-steps % DEEP, DEEP - 1 - steps)
        send(piece(here, 0, rows), piece(there, 0, rows), zs.at[way, i], zr.at[way, i], along_z[way])

    def z_forward(way, steps, c):
        if steps < far - 1:
            z_send(way, steps, chunk(c), steps * CHUNKS + c)
        elif c // (CHUNKS // 2) == way:
            first = c % (CHUNKS // 2) * CHUNK
            for k, (start, _) in enumerate(FAR):
                if first <= start < first + CHUNK:
                    z_send(way, steps, far_piece(way, k), steps * CHUNKS + k)

    def d_send(dz, rows, i):
        send(piece(dz, 0, rows), piece(dz, 1, rows), ds_.at[i], dr.at[i], partner)

    def z_arrived(way, steps, rows, i):
        dz = steps if way == 0 else DEEP - steps
        arrived(piece(dz, 0, rows), zs.at[way, i], zr.at[way, i])
        return dz

    def z_take(way, steps, c):
        dz = z_arrived(way, steps, chunk(c), (steps - 1) * CHUNKS + c)
        z_forward(way, steps, c)
        d_send(dz, chunk(c), dz * CHUNKS + c)

    def d_take(dz, rows, i):
        arrived(piece(dz, 1, rows), ds_.at[i], dr.at[i])

    def far_index(way, k):
        return DEEP * CHUNKS + way * len(FAR) + k

    def far_take(k):
        for way in (0, 1):
            z_arrived(way, far, far_piece(way, k), (far - 1) * CHUNKS + k)
            d_send(far, far_piece(way, k), far_index(way, k))
        for way in (0, 1):
            d_take(far, far_piece(way, k), far_index(way, k))

    rings = {"A": ("x", 0, 0, 0), "B": ("y", 0, 1, 1)}
    for j in range(SIDE):
        rings[("A", j)] = ("y", j, 0, 2 + j)
        rings[("B", j)] = ("x", j, 1, 2 + SIDE + j)

    def w_rows(ring, step, start, count):
        axis, j, half, _ = rings[ring]
        dx, dy = (step, j) if axis == "x" else (j, step)
        owner = up_by(y, SIDE - dy, SIDE) * SIDE + up_by(x, SIDE - dx, SIDE)
        return w.at[pl.ds(pl.multiple_of(owner * SHARD + half * HALF + start, QUARTER), count)]

    def w_send(ring, step, start, count, way, i):
        axis, _, _, r = rings[ring]
        ref = w_rows(ring, step, start, count)
        send(ref, ref, ws.at[r, i], wr.at[r, i], along[(axis, way)])

    def w_begin(ring):
        w_send(ring, 0, 0, HALF, 0, 0)
        w_send(ring, 0, 0, HALF, 1, 1)

    def w_near(ring):
        r = rings[ring][3]
        arrived(w_rows(ring, 1, 0, HALF), ws.at[r, 0], wr.at[r, 0])
        w_send(ring, 1, 0, QUARTER, 0, 2)
        arrived(w_rows(ring, SIDE - 1, 0, HALF), ws.at[r, 1], wr.at[r, 1])
        w_send(ring, SIDE - 1, QUARTER, QUARTER, 1, 3)

    def w_far(ring):
        r = rings[ring][3]
        arrived(w_rows(ring, 2, 0, QUARTER), ws.at[r, 2], wr.at[r, 2])
        arrived(w_rows(ring, 2, QUARTER, QUARTER), ws.at[r, 3], wr.at[r, 3])

    def row_of(dz, which):
        owner = up_by(z, DEEP - dz, DEEP) * 2 + (core if which == 0 else 1 - core)
        return owner * ROWS

    def project(dz, spans):
        def tile(j, carry):
            cols = pl.ds(pl.multiple_of(j * 256, 256), 256)
            mine = pl.ds(pl.multiple_of(j * 128, 128), 128)
            parts = [tok[dz, pl.ds(a, n), :] for a, n in spans]
            lhs = parts[0] if len(parts) == 1 else jnp.concatenate(parts, axis=0)
            both = jnp.dot(lhs, w[:, cols], preferred_element_type=F32)
            gate = both[:, :128] * scales[j, 0:1]
            up = both[:, 128:] * scales[j, 1:2]
            out = (gate / (1.0 + jnp.exp(-gate)) * up).astype(BF16)
            at = 0
            for a, n in spans:
                while n > 0:
                    size = min(n, ROWS - a % ROWS)
                    to = pl.multiple_of(row_of(dz, a // ROWS) + a % ROWS, 16)
                    hidden[pl.ds(to, size), mine] = out[at:at + size]
                    a, n, at = a + size, n - size, at + size
            return carry

        lax.fori_loop(0, TILES, tile, 0)

    def own_out(c):
        z_forward(0, 0, c)
        z_forward(1, 0, c)
        d_send(0, chunk(c), c)

    loads["mg"].wait()
    loads["pg"].wait()
    norm(0)
    pl.semaphore_wait(barrier, len(neighbours))
    loads["gw"].wait()
    loads["uw"].wait()
    own = pl.ds(pl.multiple_of(fs * SHARD, SHARD), SHARD)
    for j in range(TILES):
        w[own, j * 256:j * 256 + 128] = gate_v[:, j * 128:(j + 1) * 128].astype(BF16)
        w[own, j * 256 + 128:(j + 1) * 256] = up_v[:, j * 128:(j + 1) * 128].astype(BF16)

    own_out(0)
    norm(1)
    for r in ("A", "B", ("A", 0), ("B", 0)):
        w_begin(r)
    for c in range(2, CHUNKS):
        norm(c)
        own_out(c - 1)
    loads["gs"].wait()
    loads["us"].wait()
    for j in range(TILES):
        scales[j, 0] = gs[j * 128:(j + 1) * 128]
        scales[j, 1] = us[j * 128:(j + 1) * 128]
    own_out(CHUNKS - 1)

    def z_both(steps, c):
        z_take(0, steps, c)
        z_take(1, steps, c)

    w_near("A")
    w_near("B")
    for r in ("A", "B"):
        w_begin((r, 1))
        w_begin((r, 3))
    z_both(1, 0)
    w_near(("A", 0))
    w_near(("B", 0))
    w_far("A")
    w_far("B")
    w_begin(("A", 2))
    w_begin(("B", 2))
    z_both(1, 1)
    w_near(("A", 1))
    w_near(("B", 1))
    z_both(1, 2)
    w_near(("A", 3))
    w_near(("B", 3))
    w_far(("A", 0))
    w_far(("B", 0))
    z_both(1, 3)
    w_near(("A", 2))
    w_near(("B", 2))
    for j in (1, 3):
        w_far(("A", j))
        w_far(("B", j))
    z_both(2, 0)
    w_far(("A", 2))
    w_far(("B", 2))

    def whole(dz):
        for c in range(CHUNKS):
            d_take(dz, chunk(c), dz * CHUNKS + c)
        project(dz, ((0, 2 * ROWS),))

    whole(0)
    whole(1)
    z_both(2, 1)
    whole(DEEP - 1)
    z_both(2, 2)
    z_both(2, 3)
    whole(2)
    z_both(3, 0)
    whole(DEEP - 2)
    z_both(3, 1)
    z_both(3, 2)
    z_both(3, 3)
    whole(3)
    whole(DEEP - 3)
    for k in range(len(FAR)):
        far_take(k)
        project(far, tuple(
            (which * ROWS + rows[0], rows[1])
            for which in (0, 1) for rows in (far_piece(0, k), far_piece(1, k))
        ))

    for c in sent:
        c.wait_send()


def on_device(
    stream_in, mixer_out, mix_gain, pre_gain, gate_weight, up_weight, gate_scale, up_scale
):
    any_ = pl.BlockSpec(memory_space=pltpu.HBM)
    dma = pltpu.SemaphoreType.DMA
    z_copies = (DEEP // 2) * CHUNKS
    return pl.pallas_call(
        kernel,
        name="gathered_projections",
        out_shape=(
            jax.ShapeDtypeStruct((DEEP * 2 * ROWS, COLS), BF16),
            jax.ShapeDtypeStruct((ROWS, D), BF16),
        ),
        in_specs=[any_] * 8,
        out_specs=(pl.BlockSpec(memory_space=pltpu.VMEM),) * 2,
        scratch_shapes=[
            pltpu.VMEM((DEEP, 2 * ROWS, D), BF16),
            pltpu.VMEM((D, 2 * COLS), BF16),
            pltpu.VMEM((ROWS, D), BF16),
            pltpu.VMEM((ROWS, D), BF16),
            pltpu.VMEM((SHARD, COLS), F32),
            pltpu.VMEM((SHARD, COLS), F32),
            pltpu.VMEM((1, D), F32),
            pltpu.VMEM((1, D), F32),
            pltpu.VMEM((COLS,), F32),
            pltpu.VMEM((COLS,), F32),
            pltpu.VMEM((TILES, 2, 128), F32),
            dma((6 + 2 * CHUNKS,)),
            dma((2, z_copies)),
            dma((2, z_copies)),
            dma((DEEP * CHUNKS + 2 * len(FAR),)),
            dma((DEEP * CHUNKS + 2 * len(FAR),)),
            dma((2 + 2 * SIDE, 4)),
            dma((2 + 2 * SIDE, 4)),
        ],
        compiler_params=pltpu.CompilerParams(
            collective_id=0, has_side_effects=True, vmem_limit_bytes=40 * 2**20
        ),
    )(*(
        pltpu.with_memory_space_constraint(a, pltpu.HBM)
        for a in (
            stream_in, mixer_out, mix_gain.reshape(1, -1), pre_gain.reshape(1, -1),
            gate_weight, up_weight, gate_scale, up_scale,
        )
    ))


def solution(mesh):
    return jax.shard_map(
        on_device,
        mesh=mesh,
        in_specs=(
            P(("fs", "tp"), None),
            P(("fs", "tp"), None),
            P(),
            P(),
            P("fs", "tp"),
            P("fs", "tp"),
            P("tp"),
            P("tp"),
        ),
        out_specs=(P("fs", "tp"), P(("fs", "tp"), None)),
        check_vma=False,
    )
```

```python
import functools

import jax
import jax.numpy as jnp
from jax import lax
from jax.experimental import pallas as pl
from jax.experimental.pallas import tpu as pltpu
from jax.sharding import PartitionSpec as P

MESH = pl.DeviceIdType.MESH
epsilon = 1e-06

D = 4096
ROWS = 128
COLS = 384
SIDE = 4
DEEP = 8
SHARD = 256
HALF = SHARD // 2
QUARTER = HALF // 2
CHUNK = 32
CHUNKS = ROWS // CHUNK
WINDOW = DEEP // 2
WHOLE = tuple((c * CHUNK, CHUNK) for c in range(CHUNKS))
LAST = WHOLE[:-1] + ((96, 16), (112, 16))
LANES = 512
TILES = COLS // 128
F32 = jnp.float32
BF16 = jnp.bfloat16


def kernel(
    stream_in, mixer_out, mix_gain, pre_gain, gate_w, up_w, gate_s, up_s,
    hidden, stream,
    tok, transit, w0, w1, stream_v, mixer_v, gate_v, up_v, mg, pg, gs, us, gs1, us1,
    scales, given,
    in_sem, os_, or_, ts, tr, ds_, dr, xs, xr, rs, rr, ws, wr,
):
    fs, tp = lax.axis_index("fs"), lax.axis_index("tp")
    x, y = lax.rem(fs, SIDE), lax.div(fs, SIDE)
    core, z = lax.rem(tp, 2), lax.div(tp, 2)
    side = 1 - 2 * lax.rem(z, 2)

    def up_by(v, k, n):
        return lax.rem(v + k, n)

    def chip(k):
        return lax.rem(z + k * side + 2 * DEEP, DEEP)

    other = (fs, z * 2 + (1 - core))
    mate = (fs, chip(1) * 2 + core)
    outer = (fs, chip(-1) * 2 + core)
    along = {
        ("x", 0): (y * SIDE + up_by(x, 1, SIDE), tp),
        ("x", 1): (y * SIDE + up_by(x, SIDE - 1, SIDE), tp),
        ("y", 0): (up_by(y, 1, SIDE) * SIDE + x, tp),
        ("y", 1): (up_by(y, SIDE - 1, SIDE) * SIDE + x, tp),
    }
    neighbours = [mate, outer, other] + list(along.values())

    loads = {}

    def load(name, src, dst):
        c = pltpu.make_async_copy(src, dst, in_sem.at[len(loads)])
        c.start()
        loads[name] = c

    load("gw", gate_w, gate_v)
    load("uw", up_w, up_v)
    load("mg", mix_gain, mg)
    load("pg", pre_gain, pg)
    for c in range(CHUNKS):
        rows = pl.ds(c * CHUNK, CHUNK)
        load(("m", c), mixer_out.at[rows], mixer_v.at[rows])
        load(("s", c), stream_in.at[rows], stream_v.at[rows])
    load("gs", gate_s, gs)
    load("us", up_s, us)

    barrier = pltpu.get_barrier_semaphore()
    for n in neighbours:
        pl.semaphore_signal(barrier, inc=1, device_id=n, device_id_type=MESH)

    def norm(c):
        loads[("m", c)].wait()
        loads[("s", c)].wait()

        def some(i, carry):
            rows = pl.ds(pl.multiple_of(c * CHUNK + i * 16, 16), 16)
            parts = [pl.ds(k * LANES, LANES) for k in range(D // LANES)]
            total = jnp.zeros((16, LANES), F32)
            for p in parts:
                m = mixer_v[rows, p].astype(F32)
                total += m * m
            inv = lax.rsqrt(jnp.sum(total, axis=-1, keepdims=True) * (1.0 / D) + epsilon)
            total = jnp.zeros((16, LANES), F32)
            for p in parts:
                m = mixer_v[rows, p].astype(F32)
                s = (stream_v[rows, p].astype(F32) + m * inv * mg[:, p]).astype(BF16)
                stream[rows, p] = s
                s = s.astype(F32)
                total += s * s
            inv = lax.rsqrt(jnp.sum(total, axis=-1, keepdims=True) * (1.0 / D) + epsilon)
            for p in parts:
                s = stream[rows, p].astype(F32)
                tok[0, rows, p] = (s * inv * pg[:, p]).astype(BF16)
            return carry

        lax.fori_loop(0, CHUNK // 16, some, 0)

    sent = []

    def send(src, dst, ssem, rsem, device):
        c = pltpu.make_async_remote_copy(
            src_ref=src, dst_ref=dst, send_sem=ssem, recv_sem=rsem,
            device_id=device, device_id_type=MESH,
        )
        c.start()
        sent.append(c)

    def arrived(dst, ssem, rsem):
        pltpu.make_async_remote_copy(
            src_ref=dst, dst_ref=dst, send_sem=ssem, recv_sem=rsem,
            device_id=other, device_id_type=MESH,
        ).wait_recv()

    def piece(k, which, rows):
        return tok.at[k, pl.ds(which * ROWS + rows[0], rows[1])]

    def pieces(k):
        return LAST if k == WINDOW - 1 else WHOLE

    def passing(t, rows):
        return transit.at[t, pl.ds(rows[0], rows[1])]

    def to_outer(src, k, i):
        j = (k - 1) * CHUNKS + i
        send(src, piece(k, 0, pieces(k)[i]), os_.at[j], or_.at[j], outer)

    def to_mate(src, t, i):
        j = t * CHUNKS + i
        send(src, passing(t, WHOLE[i]), ts.at[j], tr.at[j], mate)

    def to_other(k, i):
        j = k * CHUNKS + i
        rows = pieces(k)[i]
        send(piece(k, 0, rows), piece(k, 1, rows), ds_.at[j], dr.at[j], other)

    def own_out(c):
        to_outer(piece(0, 0, WHOLE[c]), 1, c)
        to_mate(piece(0, 0, WHOLE[c]), 0, c)
        to_other(0, c)

    def from_outer(k, i):
        j = (k - 1) * CHUNKS + i
        arrived(piece(k, 0, pieces(k)[i]), os_.at[j], or_.at[j])
        if k == 1:
            to_mate(piece(1, 0, WHOLE[i]), 1, i)
        to_other(k, i)

    def from_mate(t, c):
        j = t * CHUNKS + c
        arrived(passing(t, WHOLE[c]), ts.at[j], tr.at[j])
        for i, rows in enumerate(pieces(t + 2)):
            if WHOLE[c][0] <= rows[0] < WHOLE[c][0] + CHUNK:
                to_outer(passing(t, rows), t + 2, i)

    def from_other(k, i):
        j = k * CHUNKS + i
        arrived(piece(k, 1, pieces(k)[i]), ds_.at[j], dr.at[j])

    weights = (w0, w1)
    rings = {"A": ("x", 0, 0, 0), "B": ("y", 0, 1, 1)}
    for j in range(SIDE):
        rings[("A", j)] = ("y", j, 0, 2 + j)
        rings[("B", j)] = ("x", j, 1, 2 + SIDE + j)

    def w_rows(m, ring, step, start, count):
        axis, j, half, _ = rings[ring]
        dx, dy = (step, j) if axis == "x" else (j, step)
        owner = up_by(y, SIDE - dy, SIDE) * SIDE + up_by(x, SIDE - dx, SIDE)
        first = pl.multiple_of(owner * SHARD + half * HALF + start, QUARTER)
        return weights[m].at[pl.ds(first, count)]

    def w_send(m, ring, step, start, count, way, i):
        axis, _, _, r = rings[ring]
        ref = w_rows(m, ring, step, start, count)
        send(ref, ref, ws.at[m, r, i], wr.at[m, r, i], along[(axis, way)])

    def w_begin(m, *names):
        for ring in names:
            w_send(m, ring, 0, 0, HALF, 0, 0)
            w_send(m, ring, 0, 0, HALF, 1, 1)

    def w_arrived(m, ring, step, start, count, i):
        r = rings[ring][3]
        arrived(w_rows(m, ring, step, start, count), ws.at[m, r, i], wr.at[m, r, i])

    def w_near(m, *names):
        for ring in names:
            w_arrived(m, ring, 1, 0, HALF, 0)
            w_send(m, ring, 1, 0, QUARTER, 0, 2)
            w_arrived(m, ring, SIDE - 1, 0, HALF, 1)
            w_send(m, ring, SIDE - 1, QUARTER, QUARTER, 1, 3)

    def w_far(m, *names):
        for ring in names:
            w_arrived(m, ring, 2, 0, QUARTER, 2)
            w_arrived(m, ring, 2, QUARTER, QUARTER, 3)

    halves = ("A", "B")

    def w_give():
        for i, ring in enumerate(halves):
            send(w_rows(0, ring, 0, 0, HALF), w_rows(1, ring, 0, 0, HALF), xs.at[i], xr.at[i], mate)

    def w_taken(i):
        arrived(w_rows(1, halves[i], 0, 0, HALF), xs.at[i], xr.at[i])

    def first_row(which):
        return (core if which == 0 else 1 - core) * ROWS

    def project(m, k, spans):
        def tile(j, carry):
            cols = pl.ds(pl.multiple_of(j * 256, 256), 256)
            mine = pl.ds(pl.multiple_of(j * 128, 128), 128)
            parts = [tok[k, pl.ds(a, n), :] for a, n in spans]
            lhs = parts[0] if len(parts) == 1 else jnp.concatenate(parts, axis=0)
            both = jnp.dot(lhs, weights[m][:, cols], preferred_element_type=F32)
            gate = both[:, :128] * scales[m, j, 0:1]
            up = both[:, 128:] * scales[m, j, 1:2]
            out = (gate / (1.0 + jnp.exp(-gate)) * up).astype(BF16)
            at = 0
            for a, n in spans:
                while n > 0:
                    size = min(n, ROWS - a % ROWS)
                    to = first_row(a // ROWS) + a % ROWS
                    if m == 0:
                        to = pl.multiple_of(chip(-k) * 2 * ROWS + to, 16)
                        hidden[pl.ds(to, size), mine] = out[at:at + size]
                    else:
                        to = pl.multiple_of(to, 16)
                        given[k, pl.ds(to, size), mine] = out[at:at + size]
                    a, n, at = a + size, n - size, at + size
            return carry

        lax.fori_loop(0, TILES, tile, 0)

    def both_cores(rows):
        return tuple((which * ROWS + rows[0], rows[1]) for which in (0, 1))

    parcels = [(k, 0, 2 * ROWS) for k in range(WINDOW - 1)]
    splits = ((0, 64), (64, 48), (112, 16))
    for rows in splits:
        parcels += [(WINDOW - 1, which * ROWS + rows[0], rows[1]) for which in (0, 1)]

    def give(i):
        k, first, count = parcels[i]
        to = pl.multiple_of(chip(-k) * 2 * ROWS + first, 16)
        send(
            given.at[k, pl.ds(first, count)], hidden.at[pl.ds(to, count)],
            rs.at[i], rr.at[i], mate,
        )

    def take(i):
        k, first, count = parcels[i]
        to = pl.multiple_of(chip(1 + k) * 2 * ROWS + first, 16)
        arrived(hidden.at[pl.ds(to, count)], rs.at[i], rr.at[i])

    loads["gw"].wait()
    loads["uw"].wait()
    own = pl.ds(pl.multiple_of(fs * SHARD, SHARD), SHARD)
    for j in range(TILES):
        w0[own, j * 256:j * 256 + 128] = gate_v[:, j * 128:(j + 1) * 128].astype(BF16)
        w0[own, j * 256 + 128:(j + 1) * 256] = up_v[:, j * 128:(j + 1) * 128].astype(BF16)
    loads["mg"].wait()
    loads["pg"].wait()
    norm(0)
    pl.semaphore_wait(barrier, len(neighbours))
    w_give()
    w_begin(0, "A", "B", ("A", 0), ("B", 0))
    own_out(0)
    for c in range(1, CHUNKS):
        norm(c)
        if c > 1:
            own_out(c - 1)
    loads["gs"].wait()
    loads["us"].wait()
    send(gs, gs1, xs.at[2], xr.at[2], mate)
    send(us, us1, xs.at[3], xr.at[3], mate)
    own_out(CHUNKS - 1)

    w_near(0, "A", "B")
    w_taken(0)
    w_begin(1, "A")
    from_outer(1, 0)
    w_taken(1)
    w_begin(1, "B", ("A", 0), ("B", 0))
    from_outer(1, 1)
    from_mate(0, 0)
    w_near(1, "A", "B")
    w_begin(1, ("A", 1), ("A", 3), ("B", 1), ("B", 3))
    arrived(gs1, xs.at[2], xr.at[2])
    arrived(us1, xs.at[3], xr.at[3])
    for m, (g, u) in enumerate(((gs, us), (gs1, us1))):
        for j in range(TILES):
            scales[m, j, 0] = g[j * 128:(j + 1) * 128]
            scales[m, j, 1] = u[j * 128:(j + 1) * 128]
    from_outer(1, 2)
    w_near(1, ("A", 0), ("B", 0))
    w_far(1, "A", "B")
    w_begin(1, ("A", 2), ("B", 2))
    from_mate(0, 1)
    from_outer(1, 3)
    w_near(1, ("A", 1), ("B", 1))
    from_mate(0, 2)
    w_near(1, ("A", 3), ("B", 3))
    from_outer(2, 0)
    from_mate(0, 3)
    w_near(1, ("A", 2), ("B", 2))
    w_begin(0, ("A", 1), ("A", 3), ("B", 1), ("B", 3))
    w_near(0, ("A", 0), ("B", 0))
    w_far(0, "A", "B")
    w_begin(0, ("A", 2), ("B", 2))
    from_outer(2, 1)
    from_mate(1, 0)
    for j in (0, 1, 3, 2):
        w_far(1, ("A", j), ("B", j))

    def all_of(k):
        for i in range(len(pieces(k))):
            from_other(k, i)

    full = ((0, 2 * ROWS),)
    all_of(0)
    project(1, 0, full)
    from_outer(2, 2)
    from_mate(1, 1)
    w_near(0, ("A", 1), ("B", 1))
    all_of(1)
    project(1, 1, full)
    give(0)
    from_outer(2, 3)
    from_mate(1, 2)
    w_near(0, ("A", 3), ("B", 3))
    all_of(2)
    project(1, 2, full)
    give(1)
    from_outer(3, 0)
    from_mate(1, 3)
    w_near(0, ("A", 2), ("B", 2))
    give(2)
    from_outer(3, 1)
    from_other(3, 0)
    from_other(3, 1)
    project(1, 3, both_cores(splits[0]))
    for j in (0, 1, 3, 2):
        w_far(0, ("A", j), ("B", j))
    give(3)
    give(4)
    project(0, 0, full)
    project(0, 1, full)
    from_outer(3, 2)
    from_outer(3, 3)
    project(0, 2, full)
    from_outer(3, 4)
    from_other(3, 2)
    from_other(3, 3)
    project(1, 3, both_cores(splits[1]))
    from_other(3, 4)
    project(1, 3, both_cores(splits[2]))
    give(5)
    give(6)
    give(7)
    give(8)
    project(0, 3, full)
    for i in range(len(parcels)):
        take(i)

    for c in sent:
        c.wait_send()


def on_device(
    stream_in, mixer_out, mix_gain, pre_gain, gate_weight, up_weight, gate_scale, up_scale
):
    any_ = pl.BlockSpec(memory_space=pltpu.HBM)
    dma = pltpu.SemaphoreType.DMA
    return pl.pallas_call(
        kernel,
        name="gathered_projections",
        out_shape=(
            jax.ShapeDtypeStruct((DEEP * 2 * ROWS, COLS), BF16),
            jax.ShapeDtypeStruct((ROWS, D), BF16),
        ),
        in_specs=[any_] * 8,
        out_specs=(pl.BlockSpec(memory_space=pltpu.VMEM),) * 2,
        scratch_shapes=[
            pltpu.VMEM((WINDOW, 2 * ROWS, D), BF16),
            pltpu.VMEM((2, ROWS, D), BF16),
            pltpu.VMEM((D, 2 * COLS), BF16),
            pltpu.VMEM((D, 2 * COLS), BF16),
            pltpu.VMEM((ROWS, D), BF16),
            pltpu.VMEM((ROWS, D), BF16),
            pltpu.VMEM((SHARD, COLS), F32),
            pltpu.VMEM((SHARD, COLS), F32),
            pltpu.VMEM((1, D), F32),
            pltpu.VMEM((1, D), F32),
            pltpu.VMEM((COLS,), F32),
            pltpu.VMEM((COLS,), F32),
            pltpu.VMEM((COLS,), F32),
            pltpu.VMEM((COLS,), F32),
            pltpu.VMEM((2, TILES, 2, 128), F32),
            pltpu.VMEM((WINDOW, 2 * ROWS, COLS), BF16),
            dma((6 + 2 * CHUNKS,)),
            dma((3 * CHUNKS + 1,)),
            dma((3 * CHUNKS + 1,)),
            dma((2 * CHUNKS,)),
            dma((2 * CHUNKS,)),
            dma((WINDOW * CHUNKS + 1,)),
            dma((WINDOW * CHUNKS + 1,)),
            dma((4,)),
            dma((4,)),
            dma((WINDOW + 5,)),
            dma((WINDOW + 5,)),
            dma((2, 2 + 2 * SIDE, 4)),
            dma((2, 2 + 2 * SIDE, 4)),
        ],
        compiler_params=pltpu.CompilerParams(
            collective_id=0, has_side_effects=True, vmem_limit_bytes=40 * 2**20
        ),
    )(*(
        pltpu.with_memory_space_constraint(a, pltpu.HBM)
        for a in (
            stream_in, mixer_out, mix_gain.reshape(1, -1), pre_gain.reshape(1, -1),
            gate_weight, up_weight, gate_scale, up_scale,
        )
    ))


def solution(mesh):
    return jax.shard_map(
        on_device,
        mesh=mesh,
        in_specs=(
            P(("fs", "tp"), None),
            P(("fs", "tp"), None),
            P(),
            P(),
            P("fs", "tp"),
            P("fs", "tp"),
            P("tp"),
            P("tp"),
        ),
        out_specs=(P("fs", "tp"), P(("fs", "tp"), None)),
        check_vma=False,
    )
```

```python
import functools

import jax
import jax.numpy as jnp
from jax import lax
from jax.experimental import pallas as pl
from jax.experimental.pallas import tpu as pltpu
from jax.sharding import PartitionSpec as P

MESH = pl.DeviceIdType.MESH
epsilon = 1e-06

D = 4096
ROWS = 128
COLS = 384
SIDE = 4
DEEP = 8
SHARD = 256
HALF = SHARD // 2
QUARTER = HALF // 2
CHUNK = 32
CHUNKS = ROWS // CHUNK
WINDOW = DEEP // 2
WHOLE = tuple((c * CHUNK, CHUNK) for c in range(CHUNKS))
LAST = WHOLE[:-1] + ((96, 16), (112, 16))
LANES = 512
TILES = COLS // 128
F32 = jnp.float32
BF16 = jnp.bfloat16


def kernel(
    stream_in, mixer_out, mix_gain, pre_gain, gate_w, up_w, gate_s, up_s,
    hidden, stream,
    tok, transit, w0, w1, stream_v, mixer_v, gate_v, up_v, mg, pg, gs, us, gs1, us1,
    scales, given, partial,
    in_sem, os_, or_, ts, tr, ds_, dr, xs, xr, rs, rr, ws, wr,
):
    fs, tp = lax.axis_index("fs"), lax.axis_index("tp")
    x, y = lax.rem(fs, SIDE), lax.div(fs, SIDE)
    core, z = lax.rem(tp, 2), lax.div(tp, 2)
    side = 1 - 2 * lax.rem(z, 2)

    def up_by(v, k, n):
        return lax.rem(v + k, n)

    def chip(k):
        return lax.rem(z + k * side + 2 * DEEP, DEEP)

    other = (fs, z * 2 + (1 - core))
    mate = (fs, chip(1) * 2 + core)
    outer = (fs, chip(-1) * 2 + core)
    along = {
        ("x", 0): (y * SIDE + up_by(x, 1, SIDE), tp),
        ("x", 1): (y * SIDE + up_by(x, SIDE - 1, SIDE), tp),
        ("y", 0): (up_by(y, 1, SIDE) * SIDE + x, tp),
        ("y", 1): (up_by(y, SIDE - 1, SIDE) * SIDE + x, tp),
    }
    neighbours = [mate, outer, other] + list(along.values())

    loads = {}

    def load(name, src, dst):
        c = pltpu.make_async_copy(src, dst, in_sem.at[len(loads)])
        c.start()
        loads[name] = c

    load("mg", mix_gain, mg)
    for c in range(CHUNKS):
        rows = pl.ds(c * CHUNK, CHUNK)
        load(("m", c), mixer_out.at[rows], mixer_v.at[rows])
        load(("s", c), stream_in.at[rows], stream_v.at[rows])
        if c == 0:
            load("pg", pre_gain, pg)
            load("gw", gate_w, gate_v)
            load("uw", up_w, up_v)
    load("gs", gate_s, gs)
    load("us", up_s, us)

    barrier = pltpu.get_barrier_semaphore()
    for n in neighbours:
        pl.semaphore_signal(barrier, inc=1, device_id=n, device_id_type=MESH)

    def norm(c):
        loads[("m", c)].wait()
        loads[("s", c)].wait()

        def some(i, carry):
            rows = pl.ds(pl.multiple_of(c * CHUNK + i * 16, 16), 16)
            parts = [pl.ds(k * LANES, LANES) for k in range(D // LANES)]
            total = jnp.zeros((16, LANES), F32)
            for p in parts:
                m = mixer_v[rows, p].astype(F32)
                total += m * m
            inv = lax.rsqrt(jnp.sum(total, axis=-1, keepdims=True) * (1.0 / D) + epsilon)
            total = jnp.zeros((16, LANES), F32)
            for p in parts:
                m = mixer_v[rows, p].astype(F32)
                s = (stream_v[rows, p].astype(F32) + m * inv * mg[:, p]).astype(BF16)
                stream[rows, p] = s
                s = s.astype(F32)
                total += s * s
            inv = lax.rsqrt(jnp.sum(total, axis=-1, keepdims=True) * (1.0 / D) + epsilon)
            for p in parts:
                s = stream[rows, p].astype(F32)
                tok[0, rows, p] = (s * inv * pg[:, p]).astype(BF16)
            return carry

        lax.fori_loop(0, CHUNK // 16, some, 0)

    sent = []

    def send(src, dst, ssem, rsem, device):
        c = pltpu.make_async_remote_copy(
            src_ref=src, dst_ref=dst, send_sem=ssem, recv_sem=rsem,
            device_id=device, device_id_type=MESH,
        )
        c.start()
        sent.append(c)

    def arrived(dst, ssem, rsem):
        pltpu.make_async_remote_copy(
            src_ref=dst, dst_ref=dst, send_sem=ssem, recv_sem=rsem,
            device_id=other, device_id_type=MESH,
        ).wait_recv()

    def piece(k, which, rows):
        return tok.at[k, pl.ds(which * ROWS + rows[0], rows[1])]

    def pieces(k):
        return LAST if k == WINDOW - 1 else WHOLE

    def passing(t, rows):
        return transit.at[t, pl.ds(rows[0], rows[1])]

    def to_outer(src, k, i):
        j = (k - 1) * CHUNKS + i
        send(src, piece(k, 0, pieces(k)[i]), os_.at[j], or_.at[j], outer)

    def to_mate(src, t, i):
        j = t * CHUNKS + i
        send(src, passing(t, WHOLE[i]), ts.at[j], tr.at[j], mate)

    def to_other(k, i):
        j = k * CHUNKS + i
        rows = pieces(k)[i]
        send(piece(k, 0, rows), piece(k, 1, rows), ds_.at[j], dr.at[j], other)

    def own_out(c):
        to_outer(piece(0, 0, WHOLE[c]), 1, c)
        to_mate(piece(0, 0, WHOLE[c]), 0, c)
        to_other(0, c)

    def from_outer(k, i):
        j = (k - 1) * CHUNKS + i
        arrived(piece(k, 0, pieces(k)[i]), os_.at[j], or_.at[j])
        if k == 1:
            to_mate(piece(1, 0, WHOLE[i]), 1, i)
        to_other(k, i)

    def from_mate(t, c):
        j = t * CHUNKS + c
        arrived(passing(t, WHOLE[c]), ts.at[j], tr.at[j])
        for i, rows in enumerate(pieces(t + 2)):
            if WHOLE[c][0] <= rows[0] < WHOLE[c][0] + CHUNK:
                to_outer(passing(t, rows), t + 2, i)

    def from_other(k, i):
        j = k * CHUNKS + i
        arrived(piece(k, 1, pieces(k)[i]), ds_.at[j], dr.at[j])

    weights = (w0, w1)
    rings = {"A": ("x", 0, 0, 0), "B": ("y", 0, 1, 1)}
    for j in range(SIDE):
        rings[("A", j)] = ("y", j, 0, 2 + j)
        rings[("B", j)] = ("x", j, 1, 2 + SIDE + j)

    def w_rows(m, ring, step, start, count):
        axis, j, half, _ = rings[ring]
        dx, dy = (step, j) if axis == "x" else (j, step)
        owner = up_by(y, SIDE - dy, SIDE) * SIDE + up_by(x, SIDE - dx, SIDE)
        first = pl.multiple_of(owner * SHARD + half * HALF + start, QUARTER)
        return weights[m].at[pl.ds(first, count)]

    def w_send(m, ring, step, start, count, way, i):
        axis, _, _, r = rings[ring]
        ref = w_rows(m, ring, step, start, count)
        send(ref, ref, ws.at[m, r, i], wr.at[m, r, i], along[(axis, way)])

    def w_begin(m, *names):
        for ring in names:
            w_send(m, ring, 0, 0, HALF, 0, 0)
            w_send(m, ring, 0, 0, HALF, 1, 1)

    def w_arrived(m, ring, step, start, count, i):
        r = rings[ring][3]
        arrived(w_rows(m, ring, step, start, count), ws.at[m, r, i], wr.at[m, r, i])

    def w_near(m, *names):
        for ring in names:
            w_arrived(m, ring, 1, 0, HALF, 0)
            w_send(m, ring, 1, 0, QUARTER, 0, 2)
            w_arrived(m, ring, SIDE - 1, 0, HALF, 1)
            w_send(m, ring, SIDE - 1, QUARTER, QUARTER, 1, 3)

    def w_far(m, *names):
        for ring in names:
            w_arrived(m, ring, 2, 0, QUARTER, 2)
            w_arrived(m, ring, 2, QUARTER, QUARTER, 3)

    halves = ("A", "B")

    def w_give():
        for i, ring in enumerate(halves):
            send(w_rows(0, ring, 0, 0, HALF), w_rows(1, ring, 0, 0, HALF), xs.at[i], xr.at[i], mate)

    def w_taken(i):
        arrived(w_rows(1, halves[i], 0, 0, HALF), xs.at[i], xr.at[i])

    full = ((0, 2 * ROWS),)

    def first_row(which):
        return (core if which == 0 else 1 - core) * ROWS

    def store(m, k, spans, j, both):
        mine = pl.ds(j * 128, 128)
        gate = both[:, :128] * scales[m, j, 0:1]
        up = both[:, 128:] * scales[m, j, 1:2]
        out = (gate / (1.0 + jnp.exp(-gate)) * up).astype(BF16)
        at = 0
        for a, n in spans:
            while n > 0:
                size = min(n, ROWS - a % ROWS)
                to = first_row(a // ROWS) + a % ROWS
                if m == 0:
                    to = pl.multiple_of(chip(-k) * 2 * ROWS + to, 16)
                    hidden[pl.ds(to, size), mine] = out[at:at + size]
                else:
                    to = pl.multiple_of(to, 16)
                    given[k, pl.ds(to, size), mine] = out[at:at + size]
                a, n, at = a + size, n - size, at + size

    def project(m, k, spans):
        for j in range(TILES):
            parts = [tok[k, pl.ds(a, n), :] for a, n in spans]
            lhs = parts[0] if len(parts) == 1 else jnp.concatenate(parts, axis=0)
            store(m, k, spans, j, jnp.dot(
                lhs, weights[m][:, j * 256:(j + 1) * 256], preferred_element_type=F32
            ))

    def features(steps):
        starts = []
        for step in steps:
            left, below = up_by(x, SIDE - step, SIDE), up_by(y, SIDE - step, SIDE)
            starts += [(i * SIDE + left) * SHARD for i in range(SIDE)]
            starts += [(below * SIDE + i) * SHARD + HALF for i in range(SIDE)]
        return [pl.ds(pl.multiple_of(f, HALF), HALF) for f in starts]

    def project_part(k, steps, last):
        for j in range(TILES):
            cols = slice(j * 256, (j + 1) * 256)
            fs_ = features(steps)
            both = jnp.dot(
                jnp.concatenate([tok[k, :, f] for f in fs_], axis=1),
                jnp.concatenate([w0[f, cols] for f in fs_], axis=0),
                preferred_element_type=F32,
            )
            if last:
                store(0, k, full, j, partial[k, :, cols] + both)
            else:
                partial[k, :, cols] = both

    def both_cores(rows):
        return tuple((which * ROWS + rows[0], rows[1]) for which in (0, 1))

    parcels = [(k, 0, 2 * ROWS) for k in range(WINDOW - 1)]
    splits = ((0, 96), (96, 32))
    for rows in splits:
        parcels += [(WINDOW - 1, which * ROWS + rows[0], rows[1]) for which in (0, 1)]

    def give(i):
        k, first, count = parcels[i]
        to = pl.multiple_of(chip(-k) * 2 * ROWS + first, 16)
        send(
            given.at[k, pl.ds(first, count)], hidden.at[pl.ds(to, count)],
            rs.at[i], rr.at[i], mate,
        )

    def take(i):
        k, first, count = parcels[i]
        to = pl.multiple_of(chip(1 + k) * 2 * ROWS + first, 16)
        arrived(hidden.at[pl.ds(to, count)], rs.at[i], rr.at[i])

    loads["mg"].wait()
    loads["pg"].wait()
    norm(0)
    loads["gw"].wait()
    loads["uw"].wait()
    own = pl.ds(pl.multiple_of(fs * SHARD, SHARD), SHARD)
    for j in range(TILES):
        w0[own, j * 256:j * 256 + 128] = gate_v[:, j * 128:(j + 1) * 128].astype(BF16)
        w0[own, j * 256 + 128:(j + 1) * 256] = up_v[:, j * 128:(j + 1) * 128].astype(BF16)
    pl.semaphore_wait(barrier, len(neighbours))
    to_outer(piece(0, 0, WHOLE[0]), 1, 0)
    w_give()
    to_mate(piece(0, 0, WHOLE[0]), 0, 0)
    to_other(0, 0)
    w_begin(0, "A", "B", ("A", 0), ("B", 0))
    for c in range(1, CHUNKS):
        norm(c)
        if c > 1:
            own_out(c - 1)
    loads["gs"].wait()
    loads["us"].wait()
    send(gs, gs1, xs.at[2], xr.at[2], mate)
    send(us, us1, xs.at[3], xr.at[3], mate)
    own_out(CHUNKS - 1)

    w_near(0, "A", "B")
    w_taken(0)
    w_begin(1, "A")
    from_outer(1, 0)
    w_taken(1)
    w_begin(1, "B", ("A", 0), ("B", 0))
    from_outer(1, 1)
    from_mate(0, 0)
    w_near(1, "A", "B")
    w_begin(1, ("A", 1), ("A", 3), ("B", 1), ("B", 3))
    arrived(gs1, xs.at[2], xr.at[2])
    arrived(us1, xs.at[3], xr.at[3])
    for m, (g, u) in enumerate(((gs, us), (gs1, us1))):
        for j in range(TILES):
            scales[m, j, 0] = g[j * 128:(j + 1) * 128]
            scales[m, j, 1] = u[j * 128:(j + 1) * 128]
    from_outer(1, 2)
    w_near(1, ("A", 0), ("B", 0))
    w_far(1, "A", "B")
    w_begin(1, ("A", 2), ("B", 2))
    from_mate(0, 1)
    from_outer(1, 3)
    w_near(1, ("A", 1), ("B", 1))
    from_mate(0, 2)
    w_near(1, ("A", 3), ("B", 3))
    from_outer(2, 0)
    from_mate(0, 3)
    w_near(1, ("A", 2), ("B", 2))
    w_begin(0, ("A", 1), ("A", 3), ("B", 1), ("B", 3))
    w_near(0, ("A", 0), ("B", 0))
    w_far(0, "A", "B")
    from_outer(2, 1)
    from_mate(1, 0)
    for j in (0, 1, 3, 2):
        w_far(1, ("A", j), ("B", j))

    def all_of(k):
        for i in range(len(pieces(k))):
            from_other(k, i)

    all_of(0)
    project(1, 0, full)
    from_outer(2, 2)
    from_mate(1, 1)
    w_near(0, ("A", 1), ("B", 1))
    w_begin(0, ("A", 2), ("B", 2))
    all_of(1)
    project(1, 1, full)
    give(0)
    from_outer(2, 3)
    from_mate(1, 2)
    w_near(0, ("A", 3), ("B", 3))
    all_of(2)
    project(1, 2, full)
    give(1)
    from_outer(3, 0)
    for j in (0, 1):
        w_far(0, ("A", j), ("B", j))
    project_part(0, (0, 1), False)
    give(2)
    from_mate(1, 3)
    project_part(1, (0, 1), False)
    w_near(0, ("A", 2), ("B", 2))
    from_outer(3, 1)
    project_part(2, (0, 1), False)
    from_outer(3, 2)
    for i in range(3):
        from_other(3, i)
    project(1, 3, both_cores(splits[0]))
    for j in (3, 2):
        w_far(0, ("A", j), ("B", j))
    project_part(0, (3, 2), True)
    from_outer(3, 3)
    give(3)
    give(4)
    project_part(1, (3, 2), True)
    project_part(2, (3, 2), True)
    from_outer(3, 4)
    from_other(3, 3)
    from_other(3, 4)
    project(1, 3, both_cores(splits[1]))
    give(5)
    give(6)
    project(0, 3, full)
    for i in range(len(parcels)):
        take(i)

    for c in sent:
        c.wait_send()


def finish(hidden, stream, hidden_out, stream_out, sems):
    copies = []
    for src, dst in ((hidden, hidden_out), (stream, stream_out)):
        rows = src.shape[0] // 4
        for i in range(4):
            part = pl.ds(i * rows, rows)
            copies.append(pltpu.make_async_copy(src.at[part], dst.at[part], sems.at[len(copies)]))
    for c in copies:
        c.start()
    for c in copies:
        c.wait()


def on_device(
    stream_in, mixer_out, mix_gain, pre_gain, gate_weight, up_weight, gate_scale, up_scale
):
    any_ = pl.BlockSpec(memory_space=pltpu.HBM)
    dma = pltpu.SemaphoreType.DMA
    hidden, stream = pl.pallas_call(
        kernel,
        name="gathered_projections",
        out_shape=(
            jax.ShapeDtypeStruct((DEEP * 2 * ROWS, COLS), BF16),
            jax.ShapeDtypeStruct((ROWS, D), BF16),
        ),
        in_specs=[any_] * 8,
        out_specs=(pl.BlockSpec(memory_space=pltpu.VMEM),) * 2,
        scratch_shapes=[
            pltpu.VMEM((WINDOW, 2 * ROWS, D), BF16),
            pltpu.VMEM((2, ROWS, D), BF16),
            pltpu.VMEM((D, 2 * COLS), BF16),
            pltpu.VMEM((D, 2 * COLS), BF16),
            pltpu.VMEM((ROWS, D), BF16),
            pltpu.VMEM((ROWS, D), BF16),
            pltpu.VMEM((SHARD, COLS), F32),
            pltpu.VMEM((SHARD, COLS), F32),
            pltpu.VMEM((1, D), F32),
            pltpu.VMEM((1, D), F32),
            pltpu.VMEM((COLS,), F32),
            pltpu.VMEM((COLS,), F32),
            pltpu.VMEM((COLS,), F32),
            pltpu.VMEM((COLS,), F32),
            pltpu.VMEM((2, TILES, 2, 128), F32),
            pltpu.VMEM((WINDOW, 2 * ROWS, COLS), BF16),
            pltpu.VMEM((WINDOW - 1, 2 * ROWS, 2 * COLS), F32),
            dma((6 + 2 * CHUNKS,)),
            dma((3 * CHUNKS + 1,)),
            dma((3 * CHUNKS + 1,)),
            dma((2 * CHUNKS,)),
            dma((2 * CHUNKS,)),
            dma((WINDOW * CHUNKS + 1,)),
            dma((WINDOW * CHUNKS + 1,)),
            dma((4,)),
            dma((4,)),
            dma((WINDOW + 3,)),
            dma((WINDOW + 3,)),
            dma((2, 2 + 2 * SIDE, 4)),
            dma((2, 2 + 2 * SIDE, 4)),
        ],
        compiler_params=pltpu.CompilerParams(
            collective_id=0, has_side_effects=True, vmem_limit_bytes=40 * 2**20
        ),
    )(*(
        pltpu.with_memory_space_constraint(a, pltpu.HBM)
        for a in (
            stream_in, mixer_out, mix_gain.reshape(1, -1), pre_gain.reshape(1, -1),
            gate_weight, up_weight, gate_scale, up_scale,
        )
    ))
    vmem = pl.BlockSpec(memory_space=pltpu.VMEM)
    return pl.pallas_call(
        finish,
        name="results_out",
        out_shape=(
            jax.ShapeDtypeStruct(hidden.shape, BF16),
            jax.ShapeDtypeStruct(stream.shape, BF16),
        ),
        in_specs=[vmem, vmem],
        out_specs=(any_, any_),
        scratch_shapes=[dma((8,))],
        compiler_params=pltpu.CompilerParams(vmem_limit_bytes=16 * 2**20),
    )(hidden, stream)


def solution(mesh):
    return jax.shard_map(
        on_device,
        mesh=mesh,
        in_specs=(
            P(("fs", "tp"), None),
            P(("fs", "tp"), None),
            P(),
            P(),
            P("fs", "tp"),
            P("fs", "tp"),
            P("tp"),
            P("tp"),
        ),
        out_specs=(P("fs", "tp"), P(("fs", "tp"), None)),
        check_vma=False,
    )
```

```python
import functools

import jax
import jax.numpy as jnp
from jax import lax
from jax.experimental import pallas as pl
from jax.experimental.pallas import tpu as pltpu
from jax.sharding import PartitionSpec as P

MESH = pl.DeviceIdType.MESH
epsilon = 1e-06

D = 4096
ROWS = 128
COLS = 384
SIDE = 4
DEEP = 8
SHARD = 256
HALF = SHARD // 2
QUARTER = HALF // 2
CHUNK = 32
CHUNKS = ROWS // CHUNK
WINDOW = DEEP // 2
WHOLE = tuple((c * CHUNK, CHUNK) for c in range(CHUNKS))
LAST = WHOLE[:-1] + ((96, 16), (112, 16))
LANES = 512
TILES = COLS // 128
F32 = jnp.float32
BF16 = jnp.bfloat16


def kernel(
    stream_in, mixer_out, mix_gain, pre_gain, gate_w, up_w, gate_s, up_s,
    hidden, stream,
    tok, transit, w0, w1, stream_v, mixer_v, gate_v, up_v, mg, pg, gs, us, gs1, us1,
    scales, given, partial,
    in_sem, os_, or_, ts, tr, ds_, dr, xs, xr, rs, rr, ws, wr,
):
    fs, tp = lax.axis_index("fs"), lax.axis_index("tp")
    x, y = lax.rem(fs, SIDE), lax.div(fs, SIDE)
    core, z = lax.rem(tp, 2), lax.div(tp, 2)
    side = 1 - 2 * lax.rem(z, 2)

    def up_by(v, k, n):
        return lax.rem(v + k, n)

    def chip(k):
        return lax.rem(z + k * side + 2 * DEEP, DEEP)

    other = (fs, z * 2 + (1 - core))
    mate = (fs, chip(1) * 2 + core)
    outer = (fs, chip(-1) * 2 + core)
    along = {
        ("x", 0): (y * SIDE + up_by(x, 1, SIDE), tp),
        ("x", 1): (y * SIDE + up_by(x, SIDE - 1, SIDE), tp),
        ("y", 0): (up_by(y, 1, SIDE) * SIDE + x, tp),
        ("y", 1): (up_by(y, SIDE - 1, SIDE) * SIDE + x, tp),
    }
    neighbours = [mate, outer, other] + list(along.values())

    loads = {}

    def load(name, src, dst):
        c = pltpu.make_async_copy(src, dst, in_sem.at[len(loads)])
        c.start()
        loads[name] = c

    load("mg", mix_gain, mg)
    for c in range(CHUNKS):
        rows = pl.ds(c * CHUNK, CHUNK)
        load(("m", c), mixer_out.at[rows], mixer_v.at[rows])
        load(("s", c), stream_in.at[rows], stream_v.at[rows])
        if c == 0:
            load("pg", pre_gain, pg)
            load("gw", gate_w, gate_v)
            load("uw", up_w, up_v)
    load("gs", gate_s, gs)
    load("us", up_s, us)

    barrier = pltpu.get_barrier_semaphore()
    for n in neighbours:
        pl.semaphore_signal(barrier, inc=1, device_id=n, device_id_type=MESH)

    def norm(c):
        loads[("m", c)].wait()
        loads[("s", c)].wait()

        def some(i, carry):
            rows = pl.ds(pl.multiple_of(c * CHUNK + i * 16, 16), 16)
            parts = [pl.ds(k * LANES, LANES) for k in range(D // LANES)]
            total = jnp.zeros((16, LANES), F32)
            for p in parts:
                m = mixer_v[rows, p].astype(F32)
                total += m * m
            inv = lax.rsqrt(jnp.sum(total, axis=-1, keepdims=True) * (1.0 / D) + epsilon)
            total = jnp.zeros((16, LANES), F32)
            for p in parts:
                m = mixer_v[rows, p].astype(F32)
                s = (stream_v[rows, p].astype(F32) + m * inv * mg[:, p]).astype(BF16)
                stream[rows, p] = s
                s = s.astype(F32)
                total += s * s
            inv = lax.rsqrt(jnp.sum(total, axis=-1, keepdims=True) * (1.0 / D) + epsilon)
            for p in parts:
                s = stream[rows, p].astype(F32)
                tok[0, rows, p] = (s * inv * pg[:, p]).astype(BF16)
            return carry

        lax.fori_loop(0, CHUNK // 16, some, 0)

    sent = []

    def send(src, dst, ssem, rsem, device):
        c = pltpu.make_async_remote_copy(
            src_ref=src, dst_ref=dst, send_sem=ssem, recv_sem=rsem,
            device_id=device, device_id_type=MESH,
        )
        c.start()
        sent.append(c)

    def arrived(dst, ssem, rsem):
        pltpu.make_async_remote_copy(
            src_ref=dst, dst_ref=dst, send_sem=ssem, recv_sem=rsem,
            device_id=other, device_id_type=MESH,
        ).wait_recv()

    def piece(k, which, rows):
        return tok.at[k, pl.ds(which * ROWS + rows[0], rows[1])]

    def pieces(k):
        return LAST if k == WINDOW - 1 else WHOLE

    def passing(t, rows):
        return transit.at[t, pl.ds(rows[0], rows[1])]

    def to_outer(src, k, i):
        j = (k - 1) * CHUNKS + i
        send(src, piece(k, 0, pieces(k)[i]), os_.at[j], or_.at[j], outer)

    def to_mate(src, t, i):
        j = t * CHUNKS + i
        send(src, passing(t, WHOLE[i]), ts.at[j], tr.at[j], mate)

    def to_other(k, i):
        j = k * CHUNKS + i
        rows = pieces(k)[i]
        send(piece(k, 0, rows), piece(k, 1, rows), ds_.at[j], dr.at[j], other)

    def own_out(c):
        to_outer(piece(0, 0, WHOLE[c]), 1, c)
        to_mate(piece(0, 0, WHOLE[c]), 0, c)
        to_other(0, c)

    def from_outer(k, i):
        j = (k - 1) * CHUNKS + i
        arrived(piece(k, 0, pieces(k)[i]), os_.at[j], or_.at[j])
        if k == 1:
            to_mate(piece(1, 0, WHOLE[i]), 1, i)
        to_other(k, i)

    def from_mate(t, c):
        j = t * CHUNKS + c
        arrived(passing(t, WHOLE[c]), ts.at[j], tr.at[j])
        for i, rows in enumerate(pieces(t + 2)):
            if WHOLE[c][0] <= rows[0] < WHOLE[c][0] + CHUNK:
                to_outer(passing(t, rows), t + 2, i)

    def from_other(k, i):
        j = k * CHUNKS + i
        arrived(piece(k, 1, pieces(k)[i]), ds_.at[j], dr.at[j])

    weights = (w0, w1)
    rings = {"A": ("x", 0, 0, 0), "B": ("y", 0, 1, 1)}
    for j in range(SIDE):
        rings[("A", j)] = ("y", j, 0, 2 + j)
        rings[("B", j)] = ("x", j, 1, 2 + SIDE + j)

    def w_rows(m, ring, step, start, count):
        axis, j, half, _ = rings[ring]
        dx, dy = (step, j) if axis == "x" else (j, step)
        owner = up_by(y, SIDE - dy, SIDE) * SIDE + up_by(x, SIDE - dx, SIDE)
        first = pl.multiple_of(owner * SHARD + half * HALF + start, QUARTER)
        return weights[m].at[pl.ds(first, count)]

    def w_send(m, ring, step, start, count, way, i):
        axis, _, _, r = rings[ring]
        ref = w_rows(m, ring, step, start, count)
        send(ref, ref, ws.at[m, r, i], wr.at[m, r, i], along[(axis, way)])

    def w_begin(m, *names):
        for ring in names:
            w_send(m, ring, 0, 0, HALF, 0, 0)
            w_send(m, ring, 0, 0, HALF, 1, 1)

    def w_arrived(m, ring, step, start, count, i):
        r = rings[ring][3]
        arrived(w_rows(m, ring, step, start, count), ws.at[m, r, i], wr.at[m, r, i])

    def w_near(m, *names):
        for ring in names:
            w_arrived(m, ring, 1, 0, HALF, 0)
            w_send(m, ring, 1, 0, QUARTER, 0, 2)
            w_arrived(m, ring, SIDE - 1, 0, HALF, 1)
            w_send(m, ring, SIDE - 1, QUARTER, QUARTER, 1, 3)

    def w_far(m, *names):
        for ring in names:
            w_arrived(m, ring, 2, 0, QUARTER, 2)
            w_arrived(m, ring, 2, QUARTER, QUARTER, 3)

    halves = ("A", "B")

    def w_give():
        for i, ring in enumerate(halves):
            send(w_rows(0, ring, 0, 0, HALF), w_rows(1, ring, 0, 0, HALF), xs.at[i], xr.at[i], mate)

    def w_taken(i):
        arrived(w_rows(1, halves[i], 0, 0, HALF), xs.at[i], xr.at[i])

    full = ((0, 2 * ROWS),)

    def first_row(which):
        return (core if which == 0 else 1 - core) * ROWS

    def store(m, k, spans, j, both):
        mine = pl.ds(j * 128, 128)
        gate = both[:, :128] * scales[m, j, 0:1]
        up = both[:, 128:] * scales[m, j, 1:2]
        out = (gate / (1.0 + jnp.exp(-gate)) * up).astype(BF16)
        at = 0
        for a, n in spans:
            while n > 0:
                size = min(n, ROWS - a % ROWS)
                to = first_row(a // ROWS) + a % ROWS
                if m == 0:
                    to = pl.multiple_of(chip(-k) * 2 * ROWS + to, 16)
                    hidden[pl.ds(to, size), mine] = out[at:at + size]
                else:
                    to = pl.multiple_of(to, 16)
                    given[k, pl.ds(to, size), mine] = out[at:at + size]
                a, n, at = a + size, n - size, at + size

    def project(m, k, spans):
        for j in range(TILES):
            parts = [tok[k, pl.ds(a, n), :] for a, n in spans]
            lhs = parts[0] if len(parts) == 1 else jnp.concatenate(parts, axis=0)
            store(m, k, spans, j, jnp.dot(
                lhs, weights[m][:, j * 256:(j + 1) * 256], preferred_element_type=F32
            ))

    def features(steps):
        starts = []
        for step in steps:
            left, below = up_by(x, SIDE - step, SIDE), up_by(y, SIDE - step, SIDE)
            starts += [(i * SIDE + left) * SHARD for i in range(SIDE)]
            starts += [(below * SIDE + i) * SHARD + HALF for i in range(SIDE)]
        return [pl.ds(pl.multiple_of(f, HALF), HALF) for f in starts]

    def project_part(k, steps, last):
        for j in range(TILES):
            cols = slice(j * 256, (j + 1) * 256)
            fs_ = features(steps)
            both = jnp.dot(
                jnp.concatenate([tok[k, :, f] for f in fs_], axis=1),
                jnp.concatenate([w0[f, cols] for f in fs_], axis=0),
                preferred_element_type=F32,
            )
            if last:
                store(0, k, full, j, partial[k, :, cols] + both)
            else:
                partial[k, :, cols] = both

    def both_cores(rows):
        return tuple((which * ROWS + rows[0], rows[1]) for which in (0, 1))

    parcels = [(k, 0, 2 * ROWS) for k in range(WINDOW - 1)]
    splits = ((0, 96), (96, 32))
    for rows in splits:
        parcels += [(WINDOW - 1, which * ROWS + rows[0], rows[1]) for which in (0, 1)]

    def give(i):
        k, first, count = parcels[i]
        to = pl.multiple_of(chip(-k) * 2 * ROWS + first, 16)
        send(
            given.at[k, pl.ds(first, count)], hidden.at[pl.ds(to, count)],
            rs.at[i], rr.at[i], mate,
        )

    def take(i):
        k, first, count = parcels[i]
        to = pl.multiple_of(chip(1 + k) * 2 * ROWS + first, 16)
        arrived(hidden.at[pl.ds(to, count)], rs.at[i], rr.at[i])

    loads["mg"].wait()
    loads["pg"].wait()
    norm(0)
    loads["gw"].wait()
    loads["uw"].wait()
    own = pl.ds(pl.multiple_of(fs * SHARD, SHARD), SHARD)
    for j in range(TILES):
        w0[own, j * 256:j * 256 + 128] = gate_v[:, j * 128:(j + 1) * 128].astype(BF16)
        w0[own, j * 256 + 128:(j + 1) * 256] = up_v[:, j * 128:(j + 1) * 128].astype(BF16)
    pl.semaphore_wait(barrier, len(neighbours))
    to_outer(piece(0, 0, WHOLE[0]), 1, 0)
    w_give()
    to_mate(piece(0, 0, WHOLE[0]), 0, 0)
    to_other(0, 0)
    w_begin(0, "A", "B", ("A", 0), ("B", 0))
    for c in range(1, CHUNKS):
        norm(c)
        if c > 1:
            own_out(c - 1)
    loads["gs"].wait()
    loads["us"].wait()
    send(gs, gs1, xs.at[2], xr.at[2], mate)
    send(us, us1, xs.at[3], xr.at[3], mate)
    own_out(CHUNKS - 1)

    w_near(0, "A", "B")
    w_taken(0)
    w_begin(1, "A")
    from_outer(1, 0)
    w_taken(1)
    w_begin(1, "B", ("A", 0), ("B", 0))
    from_outer(1, 1)
    from_mate(0, 0)
    w_near(1, "A", "B")
    w_begin(1, ("A", 1), ("A", 3), ("B", 1), ("B", 3))
    arrived(gs1, xs.at[2], xr.at[2])
    arrived(us1, xs.at[3], xr.at[3])
    for m, (g, u) in enumerate(((gs, us), (gs1, us1))):
        for j in range(TILES):
            scales[m, j, 0] = g[j * 128:(j + 1) * 128]
            scales[m, j, 1] = u[j * 128:(j + 1) * 128]
    from_outer(1, 2)
    w_near(1, ("A", 0), ("B", 0))
    w_far(1, "A", "B")
    w_begin(1, ("A", 2), ("B", 2))
    from_mate(0, 1)
    from_outer(1, 3)
    w_near(1, ("A", 1), ("B", 1))
    from_mate(0, 2)
    w_near(1, ("A", 3), ("B", 3))
    from_outer(2, 0)
    from_mate(0, 3)
    w_near(1, ("A", 2), ("B", 2))
    w_begin(0, ("A", 1), ("A", 3), ("B", 1), ("B", 3))
    w_near(0, ("A", 0), ("B", 0))
    w_far(0, "A", "B")
    from_outer(2, 1)
    from_mate(1, 0)
    for j in (0, 1, 3, 2):
        w_far(1, ("A", j), ("B", j))

    def all_of(k):
        for i in range(len(pieces(k))):
            from_other(k, i)

    all_of(0)
    project(1, 0, full)
    from_outer(2, 2)
    from_mate(1, 1)
    w_near(0, ("A", 1), ("B", 1))
    all_of(1)
    project(1, 1, full)
    give(0)
    from_outer(2, 3)
    from_mate(1, 2)
    w_near(0, ("A", 3), ("B", 3))
    w_begin(0, ("A", 2), ("B", 2))
    all_of(2)
    project(1, 2, full)
    give(1)
    from_outer(3, 0)
    give(2)
    from_mate(1, 3)
    for j in (0, 1, 3):
        w_far(0, ("A", j), ("B", j))
    project_part(0, (0, 1, 3), False)
    from_outer(3, 1)
    project_part(1, (0, 1, 3), False)
    w_near(0, ("A", 2), ("B", 2))
    project_part(2, (0, 1, 3), False)
    from_outer(3, 2)
    for i in range(3):
        from_other(3, i)
    project(1, 3, both_cores(splits[0]))
    w_far(0, ("A", 2), ("B", 2))
    project_part(0, (2,), True)
    from_outer(3, 3)
    give(3)
    give(4)
    project_part(1, (2,), True)
    from_outer(3, 4)
    project_part(2, (2,), True)
    from_other(3, 3)
    from_other(3, 4)
    project(1, 3, both_cores(splits[1]))
    give(5)
    give(6)
    project(0, 3, full)
    for i in range(len(parcels)):
        take(i)

    for c in sent:
        c.wait_send()


def finish(hidden, stream, hidden_out, stream_out, sems):
    copies = []
    for src, dst in ((hidden, hidden_out), (stream, stream_out)):
        rows = src.shape[0] // 4
        for i in range(4):
            part = pl.ds(i * rows, rows)
            copies.append(pltpu.make_async_copy(src.at[part], dst.at[part], sems.at[len(copies)]))
    for c in copies:
        c.start()
    for c in copies:
        c.wait()


def on_device(
    stream_in, mixer_out, mix_gain, pre_gain, gate_weight, up_weight, gate_scale, up_scale
):
    any_ = pl.BlockSpec(memory_space=pltpu.HBM)
    dma = pltpu.SemaphoreType.DMA
    hidden, stream = pl.pallas_call(
        kernel,
        name="gathered_projections",
        out_shape=(
            jax.ShapeDtypeStruct((DEEP * 2 * ROWS, COLS), BF16),
            jax.ShapeDtypeStruct((ROWS, D), BF16),
        ),
        in_specs=[any_] * 8,
        out_specs=(pl.BlockSpec(memory_space=pltpu.VMEM),) * 2,
        scratch_shapes=[
            pltpu.VMEM((WINDOW, 2 * ROWS, D), BF16),
            pltpu.VMEM((2, ROWS, D), BF16),
            pltpu.VMEM((D, 2 * COLS), BF16),
            pltpu.VMEM((D, 2 * COLS), BF16),
            pltpu.VMEM((ROWS, D), BF16),
            pltpu.VMEM((ROWS, D), BF16),
            pltpu.VMEM((SHARD, COLS), F32),
            pltpu.VMEM((SHARD, COLS), F32),
            pltpu.VMEM((1, D), F32),
            pltpu.VMEM((1, D), F32),
            pltpu.VMEM((COLS,), F32),
            pltpu.VMEM((COLS,), F32),
            pltpu.VMEM((COLS,), F32),
            pltpu.VMEM((COLS,), F32),
            pltpu.VMEM((2, TILES, 2, 128), F32),
            pltpu.VMEM((WINDOW, 2 * ROWS, COLS), BF16),
            pltpu.VMEM((WINDOW - 1, 2 * ROWS, 2 * COLS), F32),
            dma((6 + 2 * CHUNKS,)),
            dma((3 * CHUNKS + 1,)),
            dma((3 * CHUNKS + 1,)),
            dma((2 * CHUNKS,)),
            dma((2 * CHUNKS,)),
            dma((WINDOW * CHUNKS + 1,)),
            dma((WINDOW * CHUNKS + 1,)),
            dma((4,)),
            dma((4,)),
            dma((WINDOW + 3,)),
            dma((WINDOW + 3,)),
            dma((2, 2 + 2 * SIDE, 4)),
            dma((2, 2 + 2 * SIDE, 4)),
        ],
        compiler_params=pltpu.CompilerParams(
            collective_id=0, has_side_effects=True, vmem_limit_bytes=40 * 2**20
        ),
    )(*(
        pltpu.with_memory_space_constraint(a, pltpu.HBM)
        for a in (
            stream_in, mixer_out, mix_gain.reshape(1, -1), pre_gain.reshape(1, -1),
            gate_weight, up_weight, gate_scale, up_scale,
        )
    ))
    vmem = pl.BlockSpec(memory_space=pltpu.VMEM)
    return pl.pallas_call(
        finish,
        name="results_out",
        out_shape=(
            jax.ShapeDtypeStruct(hidden.shape, BF16),
            jax.ShapeDtypeStruct(stream.shape, BF16),
        ),
        in_specs=[vmem, vmem],
        out_specs=(any_, any_),
        scratch_shapes=[dma((8,))],
        compiler_params=pltpu.CompilerParams(vmem_limit_bytes=16 * 2**20),
    )(hidden, stream)


def solution(mesh):
    return jax.shard_map(
        on_device,
        mesh=mesh,
        in_specs=(
            P(("fs", "tp"), None),
            P(("fs", "tp"), None),
            P(),
            P(),
            P("fs", "tp"),
            P("fs", "tp"),
            P("tp"),
            P("tp"),
        ),
        out_specs=(P("fs", "tp"), P(("fs", "tp"), None)),
        check_vma=False,
    )
```
